32 devices in a mesh: grp: 2 (over y), fs: 4 (over z), tp: 4 (over x, core).
Axes of the slice: x: 2, y: 2, z: 4, core: 2. Of those that a mesh axis runs over, the one named last changes fastest.
Arguments:
- prompt_rows: bfloat16 [8192, 2048], P(('grp', 'fs')), parts along dimension 0, may hold values from -6 to 6
- up_master: float32 [2048, 8192], P('fs', 'tp'), may hold values from -0.125 to 0.125
- down_master: float32 [8192, 2048], P('fs', 'tp'), may hold values from -0.0625 to 0.0625
- norm_gain: float32 [2048], P('fs'), may hold values from 0.1 to 1.9
Outputs:
- up_sampler: bfloat16 [8, 2048, 2048], P(('grp', 'tp')), parts along dimension 0
- down_sampler: bfloat16 [8, 2048, 2048], P(('grp', 'tp')), parts along dimension 0
- layer_out: bfloat16 [8192, 2048], P(('grp', 'fs', 'tp')), parts along dimension 0
The draws below stay inside these ranges and needn't reach their ends.
There are 2 independent parts, one for each index of `grp`. The reference program is written for one: setup_inputs(seed, part) draws one part's arguments, and reference() takes and returns one part's arrays. A program takes and returns all parts, laid end to end along the dimension named above; an argument that names none is the same for every part. Nothing has to cross between parts.
All inputs are finite; a program needn't handle non-finite values.
Results may differ from the reference program's by a relative error of at most 0.014.
Values may be sent and summed in bfloat16 or wider, within the bound.
A program may use at most 128 MiB of HBM per device.

```python
import jax
import jax.numpy as jnp
from jax import lax

D = 2048
FF = 8192
TOKENS = 4096
UNIT_SPAN = 512
N_FS = 4
N_TP = 4


def block_scale(rng, extent, split, low, largest):
    level, own = 1.0, jax.random.fold_in(rng, 6)
    for dim, blocks in split:
        steps = jnp.exp(jax.random.uniform(jax.random.fold_in(own, dim), (blocks,), jnp.float32, low / len(split), largest / len(split)))
        level = level * jnp.repeat(steps, extent[dim] // blocks).reshape([-1 if axis == dim else 1 for axis in range(len(extent))])
    return level


def noise(stream_key, shape, width, reach, cuts=(), kind=jnp.bfloat16):
    gain = block_scale(stream_key, shape, cuts, -0.22, 0.18) if cuts else 1.0
    drawn = jax.random.normal(stream_key, shape, jnp.float32) * width * gain
    return jnp.minimum(jnp.maximum(drawn, -reach), reach).astype(kind)


def setup_inputs(seed: int = 0, part: int = 0) -> dict:
    key_of = jax.random.split(jax.random.key(seed), 5)
    part_splits = jax.random.split(jax.random.fold_in(key_of[4], part), 5)
    prompt_rows = noise(part_splits[0], (TOKENS, D), 1.0, 6.0, ((0, 4),))
    up_master = noise(key_of[1], (D, FF), D ** -0.5, 0.125, ((0, 4), (1, 4)), jnp.float32)
    down_master = noise(key_of[2], (FF, D), FF ** -0.5, 0.0625, ((0, 4), (1, 4)), jnp.float32)
    norm_gain = jnp.clip(1.0 + 0.18 * jax.random.normal(key_of[3], (D,), jnp.float32), 0.1, 1.9)
    return {"prompt_rows": prompt_rows, "up_master": up_master, "down_master": down_master, "norm_gain": norm_gain}


eps = 1e-06

def reference(prompt_rows, up_master, down_master, norm_gain):
    folded = (up_master * norm_gain[:, None]).astype(jnp.bfloat16)
    down_cast = down_master.astype(jnp.bfloat16)
    up_sampler = folded.reshape(D, N_FS, N_TP, UNIT_SPAN).transpose(2, 0, 1, 3).reshape(N_TP, D, N_FS * UNIT_SPAN)
    down_sampler = down_cast.reshape(N_FS, N_TP, UNIT_SPAN, D).transpose(1, 0, 2, 3).reshape(N_TP, N_FS * UNIT_SPAN, D)
    values = prompt_rows.astype(jnp.float32)
    normed = (values * lax.rsqrt(lax.optimization_barrier(jnp.mean(values * values, axis=-1, keepdims=True)) + eps)).astype(jnp.bfloat16)
    total = jnp.zeros((prompt_rows.shape[0], D), jnp.float32)
    for group in range(N_TP):
        pre_act = jnp.dot(normed, up_sampler[group], preferred_element_type=jnp.float32)
        hidden = jnp.square(jax.nn.relu(pre_act)).astype(jnp.bfloat16)
        partial_value = jnp.dot(hidden, down_sampler[group], preferred_element_type=jnp.float32).astype(jnp.bfloat16)
        partial_value = lax.optimization_barrier(partial_value)
        total = total + partial_value.astype(jnp.float32)
    return (up_sampler, down_sampler, total.astype(jnp.bfloat16))
```

```python
import functools

import jax
import jax.numpy as jnp
from jax import lax
from jax.experimental import pallas as pl
from jax.experimental.pallas import tpu as pltpu
from jax.sharding import PartitionSpec as P

eps = 1e-06
row_tile = 256
norm_tile = 64
copy_rows = 256
copy_slots = 8
MESH = pl.DeviceIdType.MESH


def gather_kernel(
    n, tp, up_cast, down_cast, rows_ref, up_out, down_out, layer_out,
    up_all, down_all, normed, hidden, part, arrived,
    local_sem, tp_send, tp_recv, z_send, z_recv, y_send, y_recv,
    sum_send, sum_recv, out_sem,
):
    y = lax.axis_index("grp")
    z = lax.axis_index("fs")
    me = lax.axis_index("tp")
    chips = tp // 2
    casts = (up_cast, down_cast)
    alls = (up_all, down_all)
    outs = (up_out, down_out)
    tokens = rows_ref.shape[0]
    share = tokens // tp

    def source(device, j):
        return lax.rem(device // 2 + j // 2, chips) * 2 + lax.rem(lax.rem(device, 2) + j % 2, 2)

    def target(j):
        return lax.rem(me // 2 + chips - j // 2, chips) * 2 + lax.rem(lax.rem(me, 2) + j % 2, 2)

    def columns(w, b):
        width = casts[w].shape[2]
        return pl.ds(pl.multiple_of(b * width, width), width)

    def block(w, a, b, h):
        depth = casts[w].shape[1]
        half = depth // 2
        return alls[w].at[pl.ds(pl.multiple_of(a * depth + h * half, half), half), columns(w, b)]

    def remote(src, dst, send, recv, device):
        return pltpu.make_async_remote_copy(
            src_ref=src, dst_ref=dst, send_sem=send, recv_sem=recv,
            device_id=device, device_id_type=MESH,
        )

    def tp_copy(w, j, k):
        h = y if k == 0 else 1 - y
        half = casts[w].shape[1] // 2
        t = target(j)
        src = casts[w].at[t, pl.ds(pl.multiple_of(h * half, half), half), :]
        return remote(src, block(w, z, me, h), tp_send.at[w, j, k], tp_recv.at[w, j, k], {"tp": t})

    def tp_arrival(w, j, k):
        h = y if k == 0 else 1 - y
        ref = block(w, z, source(me, j), h)
        return remote(ref, ref, tp_send.at[w, j, k], tp_recv.at[w, j, k], {"tp": target(j)})

    def z_copy(w, j, a, slot, device):
        ref = block(w, a, source(me, j), y)
        return remote(ref, ref, z_send.at[w, j, slot], z_recv.at[w, j, a], {"fs": device})

    def y_copy(w, j, a, h):
        ref = block(w, a, source(me, j), h)
        return remote(ref, ref, y_send.at[w, j, a], y_recv.at[w, j, a], {"grp": 1 - y})

    def local_copy(w):
        depth = casts[w].shape[1]
        dst = alls[w].at[pl.ds(pl.multiple_of(z * depth, depth), depth), columns(w, me)]
        return pltpu.make_async_copy(casts[w].at[me], dst, local_sem.at[w])

    def out_copy(w, j):
        cols = columns(w, source(me, j))
        return pltpu.make_async_copy(alls[w].at[:, cols], outs[w].at[:, cols], out_sem.at[w, j])

    def sum_copy(j, k):
        t = target(k)
        cols = columns(1, source(me, j))
        src = part.at[pl.ds(pl.multiple_of(t * share, share), share), cols]
        return remote(src, arrived.at[k - 1, :, cols], sum_send.at[j, k], sum_recv.at[j, k], {"tp": t})

    def sum_arrival(j, k):
        cols = columns(1, source(source(me, k), j))
        ref = arrived.at[k - 1, :, cols]
        return remote(ref, ref, sum_send.at[j, k], sum_recv.at[j, k], {"tp": target(k)})

    barrier = pltpu.get_barrier_semaphore()
    for j in range(1, tp):
        pl.semaphore_signal(barrier, inc=1, device_id={"tp": target(j)}, device_id_type=MESH)
    pl.semaphore_signal(barrier, inc=1, device_id={"grp": 1 - y}, device_id_type=MESH)

    @pl.when(z > 0)
    def _():
        pl.semaphore_signal(barrier, inc=1, device_id={"fs": z - 1}, device_id_type=MESH)

    @pl.when(z < n - 1)
    def _():
        pl.semaphore_signal(barrier, inc=1, device_id={"fs": z + 1}, device_id_type=MESH)

    for w in range(2):
        local_copy(w).start()
    pl.semaphore_wait(barrier, tp + (z + n - 1) // n + (2 * n - 2 - z) // n)

    for w in range(2):
        for k in range(2):
            for j in range(1, tp):
                tp_copy(w, j, k).start()

    def own_send(w, j):
        if j == 0:
            local_copy(w).wait()
        else:
            tp_arrival(w, j, 0).wait_recv()

        @pl.when(z < n - 1)
        def _():
            z_copy(w, j, z, z, z + 1).start()

        @pl.when(z > 0)
        def _():
            z_copy(w, j, z, n, z - 1).start()

    def process(w, j):
        for s in range(1, n):

            @pl.when(z - s >= 0)
            def _():
                a = z - s
                z_copy(w, j, a, a, z).wait_recv()

                @pl.when(z < n - 1)
                def _():
                    z_copy(w, j, a, a, z + 1).start()

                y_copy(w, j, a, y).start()

            @pl.when(z + s < n)
            def _():
                a = z + s
                z_copy(w, j, a, a, z).wait_recv()

                @pl.when(z > 0)
                def _():
                    z_copy(w, j, a, a, z - 1).start()

                y_copy(w, j, a, y).start()

    def finish(w, j):
        if j > 0:
            tp_arrival(w, j, 1).wait_recv()
        for a in range(n):

            @pl.when(z != a)
            def _():
                y_copy(w, j, a, 1 - y).wait_recv()

        cols = columns(w, source(me, j))
        out_copy(w, j).start()

        @pl.loop(0, tokens // row_tile)
        def _(m):
            here = pl.ds(pl.multiple_of(m * row_tile, row_tile), row_tile)
            if w == 0:
                acc = jnp.dot(normed[here, :], up_all[:, cols], preferred_element_type=jnp.float32)
                acc = jnp.maximum(acc, 0.0)
                hidden[here, cols] = (acc * acc).astype(jnp.bfloat16)
            else:
                acc = jnp.dot(hidden[here, :], down_all[:, cols], preferred_element_type=jnp.float32)
                part[here, cols] = acc.astype(jnp.bfloat16)

        if w == 1:
            for k in range(1, tp):
                sum_copy(j, k).start()

    groups = [(w, j) for w in range(2) for j in range(tp)]
    own_send(*groups[0])
    own_send(*groups[1])

    @pl.loop(0, tokens // norm_tile)
    def _(m):
        here = pl.ds(pl.multiple_of(m * norm_tile, norm_tile), norm_tile)
        values = rows_ref[here, :].astype(jnp.float32)
        scale = lax.rsqrt(jnp.mean(values * values, axis=-1, keepdims=True) + eps)
        normed[here, :] = (values * scale).astype(jnp.bfloat16)

    for g in range(len(groups)):
        process(*groups[g])
        if g + 2 < len(groups):
            own_send(*groups[g + 2])
        if g >= 1:
            finish(*groups[g - 1])
    finish(*groups[-1])

    for j in range(tp):
        for k in range(1, tp):
            sum_arrival(j, k).wait_recv()

    @pl.loop(0, share // norm_tile)
    def _(m):
        here = pl.ds(pl.multiple_of(m * norm_tile, norm_tile), norm_tile)
        mine = pl.ds(pl.multiple_of(me * share + m * norm_tile, norm_tile), norm_tile)
        total = part[mine, :].astype(jnp.float32)
        for k in range(tp - 1):
            total = total + arrived[k, here, :].astype(jnp.float32)
        layer_out[here, :] = total.astype(jnp.bfloat16)

    for w in range(2):
        for j in range(tp):
            out_copy(w, j).wait()
            if j > 0:
                for k in range(2):
                    tp_copy(w, j, k).wait_send()

            @pl.when(z > 0)
            def _():
                z_copy(w, j, z, n, z - 1).wait_send()

            for a in range(n):

                @pl.when(jnp.logical_and(a <= z, z < n - 1))
                def _():
                    z_copy(w, j, a, a, z + 1).wait_send()

                @pl.when(jnp.logical_and(a > z, z > 0))
                def _():
                    z_copy(w, j, a, a, z - 1).wait_send()

                @pl.when(z != a)
                def _():
                    y_copy(w, j, a, y).wait_send()

    for j in range(tp):
        for k in range(1, tp):
            sum_copy(j, k).wait_send()


def place_kernel(up_in, down_in, up_out, down_out, slots, in_sem, out_sem):
    jobs = []
    for src, dst in ((up_in, up_out), (down_in, down_out)):
        for first in range(0, src.shape[0], copy_rows):
            jobs.append((src.at[first : first + copy_rows, :], dst.at[first : first + copy_rows, :]))

    def load(i):
        slot = i % copy_slots
        here = slots.at[slot, :, : jobs[i][0].shape[1]]
        return pltpu.make_async_copy(jobs[i][0], here, in_sem.at[slot])

    def store(i):
        slot = i % copy_slots
        here = slots.at[slot, :, : jobs[i][0].shape[1]]
        return pltpu.make_async_copy(here, jobs[i][1], out_sem.at[slot])

    count = len(jobs)
    ahead = copy_slots // 2
    for i in range(count + ahead):
        if i < count:
            if i >= copy_slots:
                store(i - copy_slots).wait()
            load(i).start()
        if i >= ahead:
            load(i - ahead).wait()
            store(i - ahead).start()
    for i in range(max(0, count - copy_slots), count):
        store(i).wait()


def on_device(prompt_rows, up_master, down_master, norm_gain):
    n = lax.axis_size("fs")
    tp = lax.axis_size("tp")
    bf16 = jnp.bfloat16
    up_rows, width = up_master.shape
    span = width // n
    fs_per_tp = n // tp
    up_width = fs_per_tp * span
    down_width = down_master.shape[1]
    up_cast = (up_master * norm_gain[:, None]).astype(bf16)
    up_cast = up_cast.reshape(up_rows, fs_per_tp, tp, span).transpose(2, 0, 1, 3)
    up_cast = up_cast.reshape(tp, up_rows, up_width)
    down_cast = down_master.astype(bf16).reshape(tp, down_master.shape[0] // tp, down_width)
    tokens, model = prompt_rows.shape
    units = n * span
    share = tokens // tp
    vmem = pl.BlockSpec(memory_space=pltpu.VMEM)
    hbm = pl.BlockSpec(memory_space=pl.ANY)
    dma = pltpu.SemaphoreType.DMA
    up_shape = jax.ShapeDtypeStruct((model, units), bf16)
    down_shape = jax.ShapeDtypeStruct((units, model), bf16)
    up_all, down_all, layer_out = pl.pallas_call(
        functools.partial(gather_kernel, n, tp),
        out_shape=(up_shape, down_shape, jax.ShapeDtypeStruct((share, model), bf16)),
        in_specs=[vmem, vmem, vmem],
        out_specs=(hbm, hbm, vmem),
        scratch_shapes=[
            pltpu.VMEM((model, units), bf16),
            pltpu.VMEM((units, model), bf16),
            pltpu.VMEM((tokens, model), bf16),
            pltpu.VMEM((tokens, units), bf16),
            pltpu.VMEM((tokens, model), bf16),
            pltpu.VMEM((tp - 1, share, model), bf16),
            dma((2,)),
            dma((2, tp, 2)),
            dma((2, tp, 2)),
            dma((2, tp, n + 1)),
            dma((2, tp, n)),
            dma((2, tp, n)),
            dma((2, tp, n)),
            dma((tp, tp)),
            dma((tp, tp)),
            dma((2, tp)),
        ],
        compiler_params=pltpu.CompilerParams(
            collective_id=0, has_side_effects=True, vmem_limit_bytes=60 * 1024 * 1024
        ),
    )(up_cast, down_cast, prompt_rows)
    up_sampler, down_sampler = pl.pallas_call(
        place_kernel,
        out_shape=(up_shape, down_shape),
        in_specs=[hbm, hbm],
        out_specs=(hbm, hbm),
        scratch_shapes=[
            pltpu.VMEM((copy_slots, copy_rows, max(model, units)), bf16),
            dma((copy_slots,)),
            dma((copy_slots,)),
        ],
    )(up_all, down_all)
    return (up_sampler[None], down_sampler[None], layer_out)


def solution(mesh):
    in_specs = (P(("grp", "fs"), None), P("fs", "tp"), P("fs", "tp"), P("fs"))
    out_specs = (
        P(("grp", "tp"), None, None),
        P(("grp", "tp"), None, None),
        P(("grp", "fs", "tp"), None),
    )
    return jax.shard_map(
        on_device, mesh=mesh, in_specs=in_specs, out_specs=out_specs, check_vma=False
    )
```

```python
import functools

import jax
import jax.numpy as jnp
from jax import lax
from jax.experimental import pallas as pl
from jax.experimental.pallas import tpu as pltpu
from jax.sharding import PartitionSpec as P

eps = 1e-06
row_tile = 256
norm_tile = 64
copy_rows = 256
copy_slots = 8
MESH = pl.DeviceIdType.MESH


def gather_kernel(
    n, tp, cuts, up_ref, down_ref, gain_ref, rows_ref, up_out, down_out, layer_out,
    up_all, down_all, normed, hidden, part, arrived,
    up_stage, down_stage, up_cast, down_cast, gain_tall, load_sem,
    local_sem, tp_send, tp_recv, z_send, z_recv, y_send, y_recv,
    sum_send, sum_recv, out_sem,
):
    y = lax.axis_index("grp")
    z = lax.axis_index("fs")
    me = lax.axis_index("tp")
    chips = tp // 2
    depths = (up_ref.shape[0], down_ref.shape[0] // tp)
    widths = (up_ref.shape[1] // tp, down_ref.shape[1])
    alls = (up_all, down_all)
    outs = (up_out, down_out)
    tokens = rows_ref.shape[0]
    share = tokens // tp

    def source(device, j):
        return lax.rem(device // 2 + j // 2, chips) * 2 + lax.rem(lax.rem(device, 2) + j % 2, 2)

    def target(j):
        return lax.rem(me // 2 + chips - j // 2, chips) * 2 + lax.rem(lax.rem(me, 2) + j % 2, 2)

    def columns(w, b, i=None):
        if i is None:
            return pl.ds(pl.multiple_of(b * widths[w], widths[w]), widths[w])
        width = widths[w] // cuts
        return pl.ds(pl.multiple_of(b * widths[w] + i * width, width), width)

    def block(w, a, b, h, i=None):
        half = depths[w] // 2
        first = a * depths[w] + h * half
        return alls[w].at[pl.ds(pl.multiple_of(first, half), half), columns(w, b, i)]

    def cast_block(w, t, first, count):
        if w == 0:
            return up_cast.at[pl.ds(pl.multiple_of(first, count), count), columns(0, t)]
        return down_cast.at[pl.ds(pl.multiple_of(t * depths[1] + first, count), count), :]

    def remote(src, dst, send, recv, device):
        return pltpu.make_async_remote_copy(
            src_ref=src, dst_ref=dst, send_sem=send, recv_sem=recv,
            device_id=device, device_id_type=MESH,
        )

    def tp_copy(w, j, k):
        h = y if k == 0 else 1 - y
        half = depths[w] // 2
        t = target(j)
        src = cast_block(w, t, h * half, half)
        return remote(src, block(w, z, me, h), tp_send.at[w, j, k], tp_recv.at[w, j, k], {"tp": t})

    def tp_arrival(w, j, k):
        h = y if k == 0 else 1 - y
        ref = block(w, z, source(me, j), h)
        return remote(ref, ref, tp_send.at[w, j, k], tp_recv.at[w, j, k], {"tp": target(j)})

    def z_copy(w, g, a, slot, device):
        ref = block(w, a, source(me, g // cuts), y, g % cuts)
        return remote(ref, ref, z_send.at[w, g, slot], z_recv.at[w, g, a], {"fs": device})

    def y_copy(w, g, a, h):
        ref = block(w, a, source(me, g // cuts), h, g % cuts)
        return remote(ref, ref, y_send.at[w, g, a], y_recv.at[w, g, a], {"grp": 1 - y})

    def local_copy(w):
        depth = depths[w]
        dst = alls[w].at[pl.ds(pl.multiple_of(z * depth, depth), depth), columns(w, me)]
        return pltpu.make_async_copy(cast_block(w, me, 0, depth), dst, local_sem.at[w])

    def out_copy(w, j):
        cols = columns(w, source(me, j))
        return pltpu.make_async_copy(alls[w].at[:, cols], outs[w].at[:, cols], out_sem.at[w, j])

    def sum_copy(j, k):
        t = target(k)
        cols = columns(1, source(me, j // cuts), j % cuts)
        src = part.at[pl.ds(pl.multiple_of(t * share, share), share), cols]
        return remote(src, arrived.at[k - 1, :, cols], sum_send.at[j, k], sum_recv.at[j, k], {"tp": t})

    def sum_arrival(j, k):
        cols = columns(1, source(source(me, k), j // cuts), j % cuts)
        ref = arrived.at[k - 1, :, cols]
        return remote(ref, ref, sum_send.at[j, k], sum_recv.at[j, k], {"tp": target(k)})

    def up_load(h, k):
        here = pl.ds(pl.multiple_of(h * (depths[0] // 2), depths[0] // 2), depths[0] // 2)
        return pltpu.make_async_copy(up_ref.at[here, :], up_stage.at[here, :], load_sem.at[k])

    down_load = pltpu.make_async_copy(down_ref, down_stage, load_sem.at[2])
    rows_load = pltpu.make_async_copy(rows_ref, normed, load_sem.at[3])
    up_load(y, 0).start()
    up_load(1 - y, 1).start()
    down_load.start()
    rows_load.start()
    barrier = pltpu.get_barrier_semaphore()
    for j in range(1, tp):
        pl.semaphore_signal(barrier, inc=1, device_id={"tp": target(j)}, device_id_type=MESH)
    pl.semaphore_signal(barrier, inc=1, device_id={"grp": 1 - y}, device_id_type=MESH)

    @pl.when(z > 0)
    def _():
        pl.semaphore_signal(barrier, inc=1, device_id={"fs": z - 1}, device_id_type=MESH)

    @pl.when(z < n - 1)
    def _():
        pl.semaphore_signal(barrier, inc=1, device_id={"fs": z + 1}, device_id_type=MESH)

    half = depths[0] // 2
    gain_tall[...] = jnp.broadcast_to(gain_ref[...], (128, depths[0])).T

    @pl.loop(0, 2)
    def _(k):
        h = y + k - 2 * y * k
        start = pl.multiple_of(h * half, half)
        up_load(h, k).wait()

        @pl.loop(0, half // norm_tile)
        def _(m):
            here = pl.ds(pl.multiple_of(start + m * norm_tile, norm_tile), norm_tile)
            up_cast[here, :] = (up_stage[here, :] * gain_tall[here, :1]).astype(jnp.bfloat16)

    pl.semaphore_wait(barrier, tp + (z + n - 1) // n + (2 * n - 2 - z) // n)

    def own_send(w, j):
        if j == 0:
            local_copy(w).wait()
        elif j % cuts == 0:
            tp_arrival(w, j // cuts, 0).wait_recv()

        @pl.when(z < n - 1)
        def _():
            z_copy(w, j, z, z, z + 1).start()

        @pl.when(z > 0)
        def _():
            z_copy(w, j, z, n, z - 1).start()

    def process(w, j):
        for s in range(1, n):

            @pl.when(z - s >= 0)
            def _():
                a = z - s
                z_copy(w, j, a, a, z).wait_recv()

                @pl.when(z < n - 1)
                def _():
                    z_copy(w, j, a, a, z + 1).start()

                y_copy(w, j, a, y).start()

            @pl.when(z + s < n)
            def _():
                a = z + s
                z_copy(w, j, a, a, z).wait_recv()

                @pl.when(z > 0)
                def _():
                    z_copy(w, j, a, a, z - 1).start()

                y_copy(w, j, a, y).start()

    def finish(w, j):
        if j > 0 and j % cuts == 0:
            tp_arrival(w, j // cuts, 1).wait_recv()
        for a in range(n):

            @pl.when(z != a)
            def _():
                y_copy(w, j, a, 1 - y).wait_recv()

        cols = columns(w, source(me, j // cuts), j % cuts)
        if j % cuts == cuts - 1:
            out_copy(w, j // cuts).start()

        @pl.loop(0, tokens // row_tile)
        def _(m):
            here = pl.ds(pl.multiple_of(m * row_tile, row_tile), row_tile)
            if w == 0:
                acc = jnp.dot(normed[here, :], up_all[:, cols], preferred_element_type=jnp.float32)
                acc = jnp.maximum(acc, 0.0)
                hidden[here, cols] = (acc * acc).astype(jnp.bfloat16)
            else:
                acc = jnp.dot(hidden[here, :], down_all[:, cols], preferred_element_type=jnp.float32)
                part[here, cols] = acc.astype(jnp.bfloat16)

        if w == 1:
            for k in range(1, tp):
                sum_copy(j, k).start()

    def exchange(w, k):
        for j in range(1, tp):
            tp_copy(w, j, k).start()

    groups = [(w, j) for w in range(2) for j in range(tp * cuts)]
    exchange(0, 0)
    local_copy(0).start()
    for g in range(cuts):
        own_send(*groups[g])
    exchange(0, 1)
    down_load.wait()

    @pl.loop(0, down_ref.shape[0] // norm_tile)
    def _(m):
        here = pl.ds(pl.multiple_of(m * norm_tile, norm_tile), norm_tile)
        down_cast[here, :] = down_stage[here, :].astype(jnp.bfloat16)

    rows_load.wait()

    @pl.loop(0, tokens // norm_tile)
    def _(m):
        here = pl.ds(pl.multiple_of(m * norm_tile, norm_tile), norm_tile)
        values = normed[here, :].astype(jnp.float32)
        scale = lax.rsqrt(jnp.mean(values * values, axis=-1, keepdims=True) + eps)
        normed[here, :] = (values * scale).astype(jnp.bfloat16)

    exchange(1, 0)
    exchange(1, 1)
    local_copy(1).start()
    ahead = 3
    for g in range(cuts, ahead):
        own_send(*groups[g])
    for g in range(len(groups)):
        process(*groups[g])
        if g + ahead < len(groups):
            own_send(*groups[g + ahead])
        if g >= 1:
            finish(*groups[g - 1])
    finish(*groups[-1])

    for j in range(tp * cuts):
        for k in range(1, tp):
            sum_arrival(j, k).wait_recv()

    @pl.loop(0, share // norm_tile)
    def _(m):
        here = pl.ds(pl.multiple_of(m * norm_tile, norm_tile), norm_tile)
        mine = pl.ds(pl.multiple_of(me * share + m * norm_tile, norm_tile), norm_tile)
        total = part[mine, :].astype(jnp.float32)
        for k in range(tp - 1):
            total = total + arrived[k, here, :].astype(jnp.float32)
        layer_out[here, :] = total.astype(jnp.bfloat16)

    for w in range(2):
        for j in range(tp):
            out_copy(w, j).wait()
            if j > 0:
                for k in range(2):
                    tp_copy(w, j, k).wait_send()
        for j in range(tp * cuts):

            @pl.when(z > 0)
            def _():
                z_copy(w, j, z, n, z - 1).wait_send()

            for a in range(n):

                @pl.when(jnp.logical_and(a <= z, z < n - 1))
                def _():
                    z_copy(w, j, a, a, z + 1).wait_send()

                @pl.when(jnp.logical_and(a > z, z > 0))
                def _():
                    z_copy(w, j, a, a, z - 1).wait_send()

                @pl.when(z != a)
                def _():
                    y_copy(w, j, a, y).wait_send()

    for j in range(tp * cuts):
        for k in range(1, tp):
            sum_copy(j, k).wait_send()


def place_kernel(up_in, down_in, up_out, down_out, slots, in_sem, out_sem):
    jobs = []
    for src, dst in ((up_in, up_out), (down_in, down_out)):
        for first in range(0, src.shape[0], copy_rows):
            jobs.append((src.at[first : first + copy_rows, :], dst.at[first : first + copy_rows, :]))

    def load(i):
        slot = i % copy_slots
        here = slots.at[slot, :, : jobs[i][0].shape[1]]
        return pltpu.make_async_copy(jobs[i][0], here, in_sem.at[slot])

    def store(i):
        slot = i % copy_slots
        here = slots.at[slot, :, : jobs[i][0].shape[1]]
        return pltpu.make_async_copy(here, jobs[i][1], out_sem.at[slot])

    count = len(jobs)
    ahead = copy_slots // 2
    for i in range(count + ahead):
        if i < count:
            if i >= copy_slots:
                store(i - copy_slots).wait()
            load(i).start()
        if i >= ahead:
            load(i - ahead).wait()
            store(i - ahead).start()
    for i in range(max(0, count - copy_slots), count):
        store(i).wait()


def on_device(prompt_rows, up_master, down_master, norm_gain):
    n = lax.axis_size("fs")
    tp = lax.axis_size("tp")
    bf16 = jnp.bfloat16
    up_rows, width = up_master.shape
    span = width // n
    fs_per_tp = n // tp
    up_width = fs_per_tp * span
    down_width = down_master.shape[1]
    if fs_per_tp > 1:
        up_master = up_master.reshape(up_rows, fs_per_tp, tp, span).swapaxes(1, 2)
        up_master = up_master.reshape(up_rows, width)
    cuts = 2 if up_width % 256 == 0 and down_width % 256 == 0 else 1
    tokens, model = prompt_rows.shape
    units = n * span
    share = tokens // tp
    vmem = pl.BlockSpec(memory_space=pltpu.VMEM)
    hbm = pl.BlockSpec(memory_space=pl.ANY)
    dma = pltpu.SemaphoreType.DMA
    up_shape = jax.ShapeDtypeStruct((model, units), bf16)
    down_shape = jax.ShapeDtypeStruct((units, model), bf16)
    up_all, down_all, layer_out = pl.pallas_call(
        functools.partial(gather_kernel, n, tp, cuts),
        out_shape=(up_shape, down_shape, jax.ShapeDtypeStruct((share, model), bf16)),
        in_specs=[hbm, hbm, vmem, hbm],
        out_specs=(hbm, hbm, vmem),
        scratch_shapes=[
            pltpu.VMEM((model, units), bf16),
            pltpu.VMEM((units, model), bf16),
            pltpu.VMEM((tokens, model), bf16),
            pltpu.VMEM((tokens, units), bf16),
            pltpu.VMEM((tokens, model), bf16),
            pltpu.VMEM((tp - 1, share, model), bf16),
            pltpu.VMEM(up_master.shape, jnp.float32),
            pltpu.VMEM(down_master.shape, jnp.float32),
            pltpu.VMEM(up_master.shape, bf16),
            pltpu.VMEM(down_master.shape, bf16),
            pltpu.VMEM((up_rows, 128), jnp.float32),
            dma((4,)),
            dma((2,)),
            dma((2, tp, 2)),
            dma((2, tp, 2)),
            dma((2, tp * cuts, n + 1)),
            dma((2, tp * cuts, n)),
            dma((2, tp * cuts, n)),
            dma((2, tp * cuts, n)),
            dma((tp * cuts, tp)),
            dma((tp * cuts, tp)),
            dma((2, tp)),
        ],
        compiler_params=pltpu.CompilerParams(
            collective_id=0, has_side_effects=True, vmem_limit_bytes=60 * 1024 * 1024
        ),
    )(up_master, down_master, norm_gain[None, :], prompt_rows)
    up_sampler, down_sampler = pl.pallas_call(
        place_kernel,
        out_shape=(up_shape, down_shape),
        in_specs=[hbm, hbm],
        out_specs=(hbm, hbm),
        scratch_shapes=[
            pltpu.VMEM((copy_slots, copy_rows, max(model, units)), bf16),
            dma((copy_slots,)),
            dma((copy_slots,)),
        ],
    )(up_all, down_all)
    return (up_sampler[None], down_sampler[None], layer_out)


def solution(mesh):
    in_specs = (P(("grp", "fs"), None), P("fs", "tp"), P("fs", "tp"), P("fs"))
    out_specs = (
        P(("grp", "tp"), None, None),
        P(("grp", "tp"), None, None),
        P(("grp", "fs", "tp"), None),
    )
    return jax.shard_map(
        on_device, mesh=mesh, in_specs=in_specs, out_specs=out_specs, check_vma=False
    )
```

```python
import functools

import jax
import jax.numpy as jnp
from jax import lax
from jax.experimental import pallas as pl
from jax.experimental.pallas import tpu as pltpu
from jax.sharding import PartitionSpec as P

eps = 1e-06
row_tile = 256
norm_tile = 64
copy_rows = 256
MESH = pl.DeviceIdType.MESH


def gather_kernel(
    n, tp, cuts, up_ref, down_ref, gain_ref, rows_ref, up_out, down_out, layer_out,
    up_all, down_all, normed, hidden, part, arrived,
    up_stage, down_stage, up_cast, down_cast, gain_tall, load_sem,
    local_sem, tp_send, tp_recv, z_send, z_recv, y_send, y_recv,
    sum_send, sum_recv, out_sem,
):
    y = lax.axis_index("grp")
    z = lax.axis_index("fs")
    me = lax.axis_index("tp")
    chips = tp // 2
    depths = (up_ref.shape[0], down_ref.shape[0] // tp)
    widths = (up_ref.shape[1] // tp, down_ref.shape[1])
    alls = (up_all, down_all)
    outs = (up_out, down_out)
    tokens = rows_ref.shape[0]
    share = tokens // tp

    def source(device, j):
        return lax.rem(device // 2 + j // 2, chips) * 2 + lax.rem(lax.rem(device, 2) + j % 2, 2)

    def target(j):
        return lax.rem(me // 2 + chips - j // 2, chips) * 2 + lax.rem(lax.rem(me, 2) + j % 2, 2)

    def columns(w, b, i=None):
        if i is None:
            return pl.ds(pl.multiple_of(b * widths[w], widths[w]), widths[w])
        width = widths[w] // cuts
        return pl.ds(pl.multiple_of(b * widths[w] + i * width, width), width)

    def block(w, a, b, h, i=None):
        half = depths[w] // 2
        first = a * depths[w] + h * half
        return alls[w].at[pl.ds(pl.multiple_of(first, half), half), columns(w, b, i)]

    def cast_block(w, t, first, count):
        if w == 0:
            return up_cast.at[pl.ds(pl.multiple_of(first, count), count), columns(0, t)]
        return down_cast.at[pl.ds(pl.multiple_of(t * depths[1] + first, count), count), :]

    def remote(src, dst, send, recv, device):
        return pltpu.make_async_remote_copy(
            src_ref=src, dst_ref=dst, send_sem=send, recv_sem=recv,
            device_id=device, device_id_type=MESH,
        )

    def tp_copy(w, j, k):
        h = y if k == 0 else 1 - y
        half = depths[w] // 2
        t = target(j)
        src = cast_block(w, t, h * half, half)
        return remote(src, block(w, z, me, h), tp_send.at[w, j, k], tp_recv.at[w, j, k], {"tp": t})

    def tp_arrival(w, j, k):
        h = y if k == 0 else 1 - y
        ref = block(w, z, source(me, j), h)
        return remote(ref, ref, tp_send.at[w, j, k], tp_recv.at[w, j, k], {"tp": target(j)})

    def z_copy(w, g, a, slot, device):
        ref = block(w, a, source(me, g // cuts), y, g % cuts)
        return remote(ref, ref, z_send.at[w, g, slot], z_recv.at[w, g, a], {"fs": device})

    def y_copy(w, g, a, h):
        ref = block(w, a, source(me, g // cuts), h, g % cuts)
        return remote(ref, ref, y_send.at[w, g, a], y_recv.at[w, g, a], {"grp": 1 - y})

    def local_copy(w, k):
        h = y if k == 0 else 1 - y
        half = depths[w] // 2
        src = cast_block(w, me, h * half, half)
        return pltpu.make_async_copy(src, block(w, z, me, h), local_sem.at[w, k])

    def out_copy(w, j):
        cols = columns(w, source(me, j))
        return pltpu.make_async_copy(alls[w].at[:, cols], outs[w].at[:, cols], out_sem.at[w, j])

    def sum_copy(j, k):
        t = target(k)
        cols = columns(1, source(me, j // cuts), j % cuts)
        src = part.at[pl.ds(pl.multiple_of(t * share, share), share), cols]
        return remote(src, arrived.at[k - 1, :, cols], sum_send.at[j, k], sum_recv.at[j, k], {"tp": t})

    def sum_arrival(j, k):
        cols = columns(1, source(source(me, k), j // cuts), j % cuts)
        ref = arrived.at[k - 1, :, cols]
        return remote(ref, ref, sum_send.at[j, k], sum_recv.at[j, k], {"tp": target(k)})

    def up_load(h, k):
        here = pl.ds(pl.multiple_of(h * (depths[0] // 2), depths[0] // 2), depths[0] // 2)
        return pltpu.make_async_copy(up_ref.at[here, :], up_stage.at[here, :], load_sem.at[k])

    down_load = pltpu.make_async_copy(down_ref, down_stage, load_sem.at[2])
    rows_load = pltpu.make_async_copy(rows_ref, normed, load_sem.at[3])
    up_load(y, 0).start()
    up_load(1 - y, 1).start()
    down_load.start()
    rows_load.start()
    barrier = pltpu.get_barrier_semaphore()
    for j in range(1, tp):
        pl.semaphore_signal(barrier, inc=1, device_id={"tp": target(j)}, device_id_type=MESH)
    pl.semaphore_signal(barrier, inc=1, device_id={"grp": 1 - y}, device_id_type=MESH)

    @pl.when(z > 0)
    def _():
        pl.semaphore_signal(barrier, inc=1, device_id={"fs": z - 1}, device_id_type=MESH)

    @pl.when(z < n - 1)
    def _():
        pl.semaphore_signal(barrier, inc=1, device_id={"fs": z + 1}, device_id_type=MESH)

    half = depths[0] // 2
    gain_tall[...] = jnp.broadcast_to(gain_ref[...], (128, depths[0])).T

    def cast_half(k):
        h = y if k == 0 else 1 - y
        up_load(h, k).wait()

        @pl.loop(0, half // norm_tile)
        def _(m):
            first = h * half + m * norm_tile
            here = pl.ds(pl.multiple_of(first, norm_tile), norm_tile)
            up_cast[here, :] = (up_stage[here, :] * gain_tall[here, :1]).astype(jnp.bfloat16)

    cast_half(0)
    local_copy(0, 0).start()
    pl.semaphore_wait(barrier, tp + (z + n - 1) // n + (2 * n - 2 - z) // n)

    def own_send(w, j):
        if j == 0:
            local_copy(w, 0).wait()
        elif j % cuts == 0:
            tp_arrival(w, j // cuts, 0).wait_recv()

        @pl.when(z < n - 1)
        def _():
            z_copy(w, j, z, z, z + 1).start()

        @pl.when(z > 0)
        def _():
            z_copy(w, j, z, n, z - 1).start()

    def process(w, j):
        for s in range(1, n):

            @pl.when(z - s >= 0)
            def _():
                a = z - s
                z_copy(w, j, a, a, z).wait_recv()

                @pl.when(z < n - 1)
                def _():
                    z_copy(w, j, a, a, z + 1).start()

                y_copy(w, j, a, y).start()

            @pl.when(z + s < n)
            def _():
                a = z + s
                z_copy(w, j, a, a, z).wait_recv()

                @pl.when(z > 0)
                def _():
                    z_copy(w, j, a, a, z - 1).start()

                y_copy(w, j, a, y).start()

    def finish(w, j):
        if j == 0:
            local_copy(w, 1).wait()
        elif j % cuts == 0:
            tp_arrival(w, j // cuts, 1).wait_recv()
        for a in range(n):

            @pl.when(z != a)
            def _():
                y_copy(w, j, a, 1 - y).wait_recv()

        cols = columns(w, source(me, j // cuts), j % cuts)
        if j % cuts == cuts - 1:
            out_copy(w, j // cuts).start()

        @pl.loop(0, tokens // row_tile)
        def _(m):
            here = pl.ds(pl.multiple_of(m * row_tile, row_tile), row_tile)
            if w == 0:
                acc = jnp.dot(normed[here, :], up_all[:, cols], preferred_element_type=jnp.float32)
                acc = jnp.maximum(acc, 0.0)
                hidden[here, cols] = (acc * acc).astype(jnp.bfloat16)
            else:
                acc = jnp.dot(hidden[here, :], down_all[:, cols], preferred_element_type=jnp.float32)
                part[here, cols] = acc.astype(jnp.bfloat16)

        if w == 1:
            for k in range(1, tp):
                sum_copy(j, k).start()

    def exchange(w, k):
        for j in range(1, tp):
            tp_copy(w, j, k).start()

    groups = [(w, j) for w in range(2) for j in range(tp * cuts)]
    exchange(0, 0)
    for g in range(cuts):
        own_send(*groups[g])
    cast_half(1)
    local_copy(0, 1).start()
    exchange(0, 1)
    down_load.wait()

    @pl.loop(0, down_ref.shape[0] // norm_tile)
    def _(m):
        here = pl.ds(pl.multiple_of(m * norm_tile, norm_tile), norm_tile)
        down_cast[here, :] = down_stage[here, :].astype(jnp.bfloat16)

    rows_load.wait()

    @pl.loop(0, tokens // norm_tile)
    def _(m):
        here = pl.ds(pl.multiple_of(m * norm_tile, norm_tile), norm_tile)
        values = normed[here, :].astype(jnp.float32)
        scale = lax.rsqrt(jnp.mean(values * values, axis=-1, keepdims=True) + eps)
        normed[here, :] = (values * scale).astype(jnp.bfloat16)

    exchange(1, 0)
    exchange(1, 1)
    local_copy(1, 0).start()
    local_copy(1, 1).start()
    ahead = 3
    for g in range(cuts, ahead):
        own_send(*groups[g])
    for g in range(len(groups)):
        process(*groups[g])
        if g + ahead < len(groups):
            own_send(*groups[g + ahead])
        if g >= 1:
            finish(*groups[g - 1])
    finish(*groups[-1])

    for j in range(tp * cuts):
        for k in range(1, tp):
            sum_arrival(j, k).wait_recv()

    @pl.loop(0, share // norm_tile)
    def _(m):
        here = pl.ds(pl.multiple_of(m * norm_tile, norm_tile), norm_tile)
        mine = pl.ds(pl.multiple_of(me * share + m * norm_tile, norm_tile), norm_tile)
        total = part[mine, :].astype(jnp.float32)
        for k in range(tp - 1):
            total = total + arrived[k, here, :].astype(jnp.float32)
        layer_out[here, :] = total.astype(jnp.bfloat16)

    for w in range(2):
        for j in range(tp):
            out_copy(w, j).wait()
            if j > 0:
                for k in range(2):
                    tp_copy(w, j, k).wait_send()
        for j in range(tp * cuts):

            @pl.when(z > 0)
            def _():
                z_copy(w, j, z, n, z - 1).wait_send()

            for a in range(n):

                @pl.when(jnp.logical_and(a <= z, z < n - 1))
                def _():
                    z_copy(w, j, a, a, z + 1).wait_send()

                @pl.when(jnp.logical_and(a > z, z > 0))
                def _():
                    z_copy(w, j, a, a, z - 1).wait_send()

                @pl.when(z != a)
                def _():
                    y_copy(w, j, a, y).wait_send()

    for j in range(tp * cuts):
        for k in range(1, tp):
            sum_copy(j, k).wait_send()


def place_kernel(up_in, down_in, layer_in, up_out, down_out, layer_out, *scratch):
    up_slots, down_slots, layer_slots, in_sem, out_sem = scratch
    arrays = (
        (up_in, up_slots, up_out),
        (down_in, down_slots, down_out),
        (layer_in, layer_slots, layer_out),
    )
    loads, stores = [], []
    for src, slots, dst in arrays:
        for first in range(0, src.shape[0], copy_rows):
            here = slice(first, min(first + copy_rows, src.shape[0]))
            i = len(loads)
            loads.append(pltpu.make_async_copy(src.at[here, :], slots.at[here, :], in_sem.at[i]))
            stores.append(pltpu.make_async_copy(slots.at[here, :], dst.at[here, :], out_sem.at[i]))
    for load in loads:
        load.start()
    for load, store in zip(loads, stores):
        load.wait()
        store.start()
    for store in stores:
        store.wait()


def on_device(prompt_rows, up_master, down_master, norm_gain):
    n = lax.axis_size("fs")
    tp = lax.axis_size("tp")
    bf16 = jnp.bfloat16
    up_rows, width = up_master.shape
    span = width // n
    fs_per_tp = n // tp
    up_width = fs_per_tp * span
    down_width = down_master.shape[1]
    if fs_per_tp > 1:
        up_master = up_master.reshape(up_rows, fs_per_tp, tp, span).swapaxes(1, 2)
        up_master = up_master.reshape(up_rows, width)
    cuts = 2 if up_width % 256 == 0 and down_width % 256 == 0 else 1
    tokens, model = prompt_rows.shape
    units = n * span
    share = tokens // tp
    vmem = pl.BlockSpec(memory_space=pltpu.VMEM)
    hbm = pl.BlockSpec(memory_space=pl.ANY)
    dma = pltpu.SemaphoreType.DMA
    up_shape = jax.ShapeDtypeStruct((model, units), bf16)
    down_shape = jax.ShapeDtypeStruct((units, model), bf16)
    up_all, down_all, layer_out = pl.pallas_call(
        functools.partial(gather_kernel, n, tp, cuts),
        out_shape=(up_shape, down_shape, jax.ShapeDtypeStruct((share, model), bf16)),
        in_specs=[hbm, hbm, vmem, hbm],
        out_specs=(hbm, hbm, vmem),
        scratch_shapes=[
            pltpu.VMEM((model, units), bf16),
            pltpu.VMEM((units, model), bf16),
            pltpu.VMEM((tokens, model), bf16),
            pltpu.VMEM((tokens, units), bf16),
            pltpu.VMEM((tokens, model), bf16),
            pltpu.VMEM((tp - 1, share, model), bf16),
            pltpu.VMEM(up_master.shape, jnp.float32),
            pltpu.VMEM(down_master.shape, jnp.float32),
            pltpu.VMEM(up_master.shape, bf16),
            pltpu.VMEM(down_master.shape, bf16),
            pltpu.VMEM((up_rows, 128), jnp.float32),
            dma((4,)),
            dma((2, 2)),
            dma((2, tp, 2)),
            dma((2, tp, 2)),
            dma((2, tp * cuts, n + 1)),
            dma((2, tp * cuts, n)),
            dma((2, tp * cuts, n)),
            dma((2, tp * cuts, n)),
            dma((tp * cuts, tp)),
            dma((tp * cuts, tp)),
            dma((2, tp)),
        ],
        compiler_params=pltpu.CompilerParams(
            collective_id=0, has_side_effects=True, vmem_limit_bytes=60 * 1024 * 1024
        ),
    )(up_master, down_master, norm_gain[None, :], prompt_rows)
    layer_shape = jax.ShapeDtypeStruct((share, model), bf16)
    moved = (up_shape, down_shape, layer_shape)
    jobs = sum(-(-shape.shape[0] // copy_rows) for shape in moved)
    up_sampler, down_sampler, layer_out = pl.pallas_call(
        place_kernel,
        out_shape=moved,
        in_specs=[hbm, hbm, hbm],
        out_specs=(hbm, hbm, hbm),
        scratch_shapes=[
            *(pltpu.VMEM(shape.shape, bf16) for shape in moved),
            dma((jobs,)),
            dma((jobs,)),
        ],
    )(up_all, down_all, layer_out)
    return (up_sampler[None], down_sampler[None], layer_out)


def solution(mesh):
    in_specs = (P(("grp", "fs"), None), P("fs", "tp"), P("fs", "tp"), P("fs"))
    out_specs = (
        P(("grp", "tp"), None, None),
        P(("grp", "tp"), None, None),
        P(("grp", "fs", "tp"), None),
    )
    return jax.shard_map(
        on_device, mesh=mesh, in_specs=in_specs, out_specs=out_specs, check_vma=False
    )
```
